1024 devices in a mesh: fs: 32 (over z, core), tp: 32 (over y, x).
Axes of the slice: x: 4, y: 8, z: 16, core: 2. Of those that a mesh axis runs over, the one named last changes fastest.
Arguments:
- tokens: bfloat16 [16384, 4096], P('fs', 'tp'), may hold values from -16 to 16
- norm_gain: float32 [4096], P('fs'), may hold values from 0.1 to 1.9
- gate_train: float32 [4096, 12288], P('fs', 'tp'), may hold values from -6 to 6
- up_train: float32 [4096, 12288], P('fs', 'tp'), may hold values from -6 to 6
Outputs:
- gate_serve: bfloat16 [4096, 12288], P(None, 'tp')
- up_serve: bfloat16 [4096, 12288], P(None, 'tp')
- hidden: bfloat16 [16384, 12288], P('fs', 'tp')
The draws below stay inside these ranges and needn't reach their ends.
All inputs are finite; a program needn't handle non-finite values.
Results may differ from the reference program's by a relative error of at most 0.0071.
Values may be sent and summed in bfloat16 or wider, within the bound.
No kernel may reach another device: no remote copies, remote signals or barrier semaphores. Data moves between devices by JAX's collectives and lax.ppermute only.
A program may use at most 64 MiB of HBM per device.

```python
import jax
import jax.numpy as jnp
from jax import lax

D = 4096
FF = 12288
TOKENS = 16384


def steps_of(rng, extent, split, low, largest):
    loudness, own = 1.0, jax.random.fold_in(rng, 6)
    for position, parts in split:
        heights = jnp.exp(jax.random.uniform(jax.random.fold_in(own, position), (parts,), jnp.float32, low / len(split), largest / len(split)))
        loudness = loudness * jnp.repeat(heights, extent[position] // parts).reshape([-1 if axis == position else 1 for axis in range(len(extent))])
    return loudness


def scatter_about(key, dims, width, reach, cuts=(), held_as=jnp.bfloat16):
    values = jax.random.normal(key, dims, jnp.float32) * width
    if len(cuts) > 0:
        values = steps_of(key, dims, cuts, -0.22, 0.18) * values
    return jnp.clip(values, min=-reach, max=reach).astype(held_as)


def setup_inputs(seed: int = 0) -> dict:
    keys = jax.random.split(jax.random.key(seed), 5)
    tokens = scatter_about(keys[0], (TOKENS, D), 3.0, 16.0, ((0, 32), (1, 32)))
    norm_gain = jnp.clip(1.0 + 0.18 * jax.random.normal(keys[1], (D,), jnp.float32), 0.1, 1.9)
    gate_train = scatter_about(keys[2], (D, FF), 1.0, 6.0, ((0, 32), (1, 32)), jnp.float32)
    up_train = scatter_about(keys[3], (D, FF), 1.0, 6.0, ((0, 32), (1, 32)), jnp.float32)
    return dict(tokens=tokens, norm_gain=norm_gain, gate_train=gate_train, up_train=up_train)


def reference(tokens, norm_gain, gate_train, up_train):
    gain = norm_gain.astype(jnp.float32)[:, None]
    gate_serve = (gate_train * gain).astype(jnp.bfloat16)
    up_serve = (up_train * gain).astype(jnp.bfloat16)
    values = tokens.astype(jnp.float32)
    normed = (values * jax.lax.rsqrt(lax.optimization_barrier(jnp.mean(values * values, axis=-1, keepdims=True)) + 1e-06)).astype(jnp.bfloat16)
    scale = D ** (-0.5)
    gate = jnp.dot(normed, gate_serve, preferred_element_type=jnp.float32) * scale
    up = jnp.dot(normed, up_serve, preferred_element_type=jnp.float32) * scale
    hidden = (jax.nn.silu(gate) * up).astype(jnp.bfloat16)
    return (gate_serve, up_serve, hidden)
```

```python
import jax
import jax.numpy as jnp
from jax import lax
from jax.experimental import pallas as pl
from jax.experimental.pallas import tpu as pltpu
from jax.sharding import Mesh
from jax.sharding import PartitionSpec as P


NZ, NY, NX = 16, 8, 4
ROWS_P = 208
BLOCK = 128
GROUP = 8
KEPT = 2


def pairs_of(n, kind):
    return [(i, (i ^ 1) if kind == 0 else ((i - 1) % n if i % 2 == 0 else (i + 1) % n)) for i in range(n)]


def spread_y(own, kind):
    first = lax.ppermute(own, "y", pairs_of(NY, kind))
    pair = jnp.concatenate([own, first], 0)
    second = lax.ppermute(pair, "y", pairs_of(NY, 1 - kind))
    third = lax.ppermute(second, "y", pairs_of(NY, kind))
    fourth = lax.ppermute(third, "y", pairs_of(NY, 1 - kind))
    return [pair, second, third, fourth]


def partner(v, n, kind):
    odd = lax.rem(v, 2)
    return v + 1 - 2 * odd if kind == 0 else lax.rem(v + n - 1 + 2 * odd, n)


def y_order(y, kind):
    f = lambda v: partner(v, NY, kind)
    g = lambda v: partner(v, NY, 1 - kind)
    heads = [y, g(y), g(f(y)), g(f(g(y)))]
    return [v for head in heads for v in (head, f(head))]


def x_order(x):
    far = partner(x, NX, 1)
    return [x, partner(x, NX, 0), far, partner(far, NX, 0)]


def round_kernel(gate_ref, up_ref, gain_ref, out_ref):
    width = gate_ref.shape[1]
    gain = jnp.transpose(jnp.broadcast_to(gain_ref[...], (BLOCK, BLOCK)))
    for n in range(width // BLOCK):
        lanes = pl.ds(n * BLOCK, BLOCK)
        out_ref[:, lanes] = (gate_ref[:, lanes] * gain).astype(out_ref.dtype)
        out_ref[:, pl.ds(width + n * BLOCK, BLOCK)] = (up_ref[:, lanes] * gain).astype(out_ref.dtype)


def rounded(gate, up, gain):
    vmem = pl.BlockSpec(memory_space=pltpu.VMEM)
    return pl.pallas_call(
        round_kernel,
        out_shape=jax.ShapeDtypeStruct((gate.shape[0], 2 * gate.shape[1]), jnp.bfloat16),
        in_specs=[vmem] * 3,
        out_specs=vmem,
        cost_estimate=pl.CostEstimate(flops=2 * gate.size, bytes_accessed=12 * gate.size, transcendentals=0),
        name="round",
    )(gate, up, gain[None, :])


def place_kernel(n_q, *refs):
    q_refs, refs = refs[:n_q], refs[n_q:]
    *p_refs, kept, tok_out, square, tok, sem = refs
    y, x = lax.axis_index("y"), lax.axis_index("x")
    rows_p = p_refs[0].shape[1]
    square[...] = jnp.zeros_like(square)

    def place(ref, at, row, ty, tx):
        t = ty * NX + tx
        lane = pl.multiple_of(lax.rem(t, GROUP) * BLOCK, BLOCK)
        value = ref[at]
        span = pl.ds(row, value.shape[0])
        tok[lax.div(t, GROUP), span, pl.ds(lane, BLOCK)] = value
        wide = value.astype(jnp.float32)
        square[span, :] += wide * wide

    xs = x_order(x)
    ys = y_order(y, 0)
    for i, r in enumerate(q_refs):
        for j in range(NY):
            place(r, j, rows_p, ys[j], xs[i])
    ys = y_order(y, 1)
    at = 0
    for r in p_refs:
        for j in range(r.shape[0]):
            place(r, j, 0, ys[(at + j) // NX], xs[(at + j) % NX])
        at += r.shape[0]
    copy = pltpu.make_async_copy(tok.at[pl.ds(KEPT, tok_out.shape[0])], tok_out, sem)
    copy.start()
    kept[...] = tok[:KEPT]
    copy.wait()


def place_tokens(q, p, rows):
    vmem = pl.BlockSpec(memory_space=pltpu.VMEM)
    shape = (NY * NX // GROUP, rows, GROUP * BLOCK)
    return pl.pallas_call(
        lambda *refs: place_kernel(len(q), *refs),
        out_shape=(
            jax.ShapeDtypeStruct((KEPT, *shape[1:]), jnp.bfloat16),
            jax.ShapeDtypeStruct((shape[0] - KEPT, *shape[1:]), jnp.bfloat16),
            jax.ShapeDtypeStruct((rows, BLOCK), jnp.float32),
        ),
        in_specs=[vmem] * (len(q) + len(p)),
        out_specs=(vmem, pl.BlockSpec(memory_space=pltpu.HBM), vmem),
        scratch_shapes=[pltpu.VMEM(shape, jnp.bfloat16), pltpu.SemaphoreType.DMA],
        cost_estimate=pl.CostEstimate(flops=2 * rows * 4096, bytes_accessed=2 * rows * 4096, transcendentals=0),
        compiler_params=pltpu.CompilerParams(vmem_limit_bytes=8 * 1024 * 1024),
        name="place",
    )(*q, *p)


def last_kernel(w_ref, kept, tok_ref, square, gate_out, up_out, hidden_ref, held, tok, acc, sems):
    width = hidden_ref.shape[1]
    pieces, span = NY * NX // GROUP, GROUP * BLOCK
    loads, stores = [[] for _ in range(pieces)], []
    for n in range(pieces):
        rows = pl.ds(n * span, span)
        loads[n].append(pltpu.make_async_copy(w_ref.at[rows], held.at[rows], sems.at[4 * n]))
        if n >= KEPT:
            loads[n].append(
                pltpu.make_async_copy(tok_ref.at[n - KEPT], tok.at[n - KEPT], sems.at[4 * n + 1])
            )
        for m, out in enumerate((gate_out, up_out)):
            stores.append(
                pltpu.make_async_copy(
                    held.at[rows, pl.ds(m * width, width)], out.at[rows], sems.at[4 * n + 2 + m]
                )
            )
    for group in loads:
        for copy in group:
            copy.start()
    depth = w_ref.shape[0]
    norm = lax.rsqrt(jnp.sum(square[...], axis=1, keepdims=True) / depth + 1e-06) * depth ** (-0.5)
    for n in range(pieces):
        for copy in loads[n]:
            copy.wait()
        for copy in stores[2 * n : 2 * n + 2]:
            copy.start()
        features = kept[n] if n < KEPT else tok[n - KEPT]
        product = jnp.dot(features, held[pl.ds(n * span, span), :], preferred_element_type=jnp.float32)
        if n == 0:
            acc[...] = product
        elif n < pieces - 1:
            acc[...] += product
        else:
            product = acc[...] + product
            gate = product[:, :width] * norm
            up = product[:, width:] * norm
            hidden_ref[...] = (gate / (1.0 + jnp.exp(-gate)) * up).astype(hidden_ref.dtype)
    for copy in stores:
        copy.wait()


def last_part(gathered, kept, tok, square):
    depth, both = gathered.shape
    rows, width = square.shape[0], both // 2
    vmem = pl.BlockSpec(memory_space=pltpu.VMEM)
    hbm = pl.BlockSpec(memory_space=pltpu.HBM)
    return pl.pallas_call(
        last_kernel,
        out_shape=(
            jax.ShapeDtypeStruct((depth, width), jnp.bfloat16),
            jax.ShapeDtypeStruct((depth, width), jnp.bfloat16),
            jax.ShapeDtypeStruct((rows, width), jnp.bfloat16),
        ),
        in_specs=[hbm, vmem, hbm, vmem],
        out_specs=(hbm, hbm, vmem),
        scratch_shapes=[
            pltpu.VMEM((depth, both), jnp.bfloat16),
            pltpu.VMEM(tok.shape, jnp.bfloat16),
            pltpu.VMEM((rows, both), jnp.float32),
            pltpu.SemaphoreType.DMA((32,)),
        ],
        cost_estimate=pl.CostEstimate(
            flops=4 * rows * depth * width, bytes_accessed=6 * depth * both, transcendentals=rows * width
        ),
        compiler_params=pltpu.CompilerParams(vmem_limit_bytes=51 * 1024 * 1024),
        name="last",
    )(gathered, kept, tok, square)


def inner(tokens, norm_gain, gate_train, up_train):
    own = rounded(gate_train, up_train, norm_gain)
    gathered = lax.all_gather(own, ("z", "c"), axis=0, tiled=True)

    p0, q0 = tokens[None, :ROWS_P], tokens[None, ROWS_P:]
    pair = jnp.concatenate([p0, lax.ppermute(p0, "x", pairs_of(NX, 0))], 0)
    p4 = jnp.concatenate([pair, lax.ppermute(pair, "x", pairs_of(NX, 1))], 0)
    p = spread_y(p4, 1)
    q8 = jnp.concatenate(spread_y(q0, 0), 0)
    qa = lax.ppermute(q8, "x", pairs_of(NX, 0))
    qb = lax.ppermute(q8, "x", pairs_of(NX, 1))
    qc = lax.ppermute(qb, "x", pairs_of(NX, 0))
    kept, tok, square = place_tokens([q8, qa, qb, qc], p, tokens.shape[0])
    return last_part(gathered, kept, tok, square)


def solution(mesh):
    split = Mesh(mesh.devices.reshape(NZ, 2, NY, NX), ("z", "c", "y", "x"))
    fs, tp = ("z", "c"), ("y", "x")
    placed = (P(fs, tp), P(fs), P(fs, tp), P(fs, tp))
    return jax.shard_map(
        inner,
        mesh=split,
        in_specs=placed,
        out_specs=(P(None, tp), P(None, tp), P(fs, tp)),
        check_vma=False,
    )
```

```python
import jax
import jax.numpy as jnp
from jax import lax
from jax.experimental import pallas as pl
from jax.experimental.pallas import tpu as pltpu
from jax.sharding import Mesh
from jax.sharding import PartitionSpec as P


NZ, NY, NX = 16, 8, 4
ROWS_P = 256
BLOCK = 128
LIMIT_A, LIMIT_B = 51, 20
GROUP = 8
HALF = 2


def pairs_of(n, kind):
    return [(i, (i ^ 1) if kind == 0 else ((i - 1) % n if i % 2 == 0 else (i + 1) % n)) for i in range(n)]


SWAP = [(0, 1), (1, 0)]


def spread_y(own, kind):
    first = lax.ppermute(own, "y", pairs_of(NY, kind))
    pair = jnp.concatenate([own, first], 0)
    second = lax.ppermute(pair, "y", pairs_of(NY, 1 - kind))
    third = lax.ppermute(second, "y", pairs_of(NY, kind))
    fourth = lax.ppermute(third, "y", pairs_of(NY, 1 - kind))
    return [pair, second, third, fourth]


def partner(v, n, kind):
    odd = lax.rem(v, 2)
    return v + 1 - 2 * odd if kind == 0 else lax.rem(v + n - 1 + 2 * odd, n)


def y_order(y, kind):
    f = lambda v: partner(v, NY, kind)
    g = lambda v: partner(v, NY, 1 - kind)
    heads = [y, g(y), g(f(y)), g(f(g(y)))]
    return [v for head in heads for v in (head, f(head))]


def x_order(x):
    far = partner(x, NX, 1)
    return [x, partner(x, NX, 0), far, partner(far, NX, 0)]


def round_kernel(gate_ref, up_ref, gain_ref, out_ref):
    width = gate_ref.shape[1]
    gain = jnp.transpose(jnp.broadcast_to(gain_ref[...], (BLOCK, BLOCK)))
    for n in range(width // BLOCK):
        lanes = pl.ds(n * BLOCK, BLOCK)
        out_ref[:, lanes] = (gate_ref[:, lanes] * gain).astype(out_ref.dtype)
        out_ref[:, pl.ds(width + n * BLOCK, BLOCK)] = (up_ref[:, lanes] * gain).astype(out_ref.dtype)


def rounded(gate, up, gain):
    vmem = pl.BlockSpec(memory_space=pltpu.VMEM)
    return pl.pallas_call(
        round_kernel,
        out_shape=jax.ShapeDtypeStruct((gate.shape[0], 2 * gate.shape[1]), jnp.bfloat16),
        in_specs=[vmem] * 3,
        out_specs=vmem,
        cost_estimate=pl.CostEstimate(flops=2 * gate.size, bytes_accessed=12 * gate.size, transcendentals=0),
        name="round",
    )(gate, up, gain[None, :])


def place_kernel(n_q, *refs):
    q_refs, refs = refs[:n_q], refs[n_q:]
    *p_refs, first, second, square, tok, sem = refs
    c, y, x = lax.axis_index("c"), lax.axis_index("y"), lax.axis_index("x")
    rows_p = p_refs[0].shape[1]
    square[...] = jnp.zeros_like(square)

    def place(ref, at, row, ty, tx):
        t = ty * NX + tx
        far = jnp.where(lax.rem(t, 2) == c, 0, HALF)
        group = far + lax.div(t, 2 * GROUP)
        lane = pl.multiple_of(lax.rem(lax.div(t, 2), GROUP) * BLOCK, BLOCK)
        value = ref[at]
        span = pl.ds(row, value.shape[0])
        tok[group, span, pl.ds(lane, BLOCK)] = value
        wide = value.astype(jnp.float32)
        square[span, :] += wide * wide

    xs = x_order(x)
    ys = y_order(y, 0)
    for i, r in enumerate(q_refs):
        for j in range(NY):
            place(r, j, rows_p, ys[j], xs[i])
    ys = y_order(y, 1)
    at = 0
    for r in p_refs:
        for j in range(r.shape[0]):
            place(r, j, 0, ys[(at + j) // NX], xs[(at + j) % NX])
        at += r.shape[0]
    copy = pltpu.make_async_copy(tok.at[pl.ds(0, HALF)], first, sem)
    copy.start()
    second[...] = tok[HALF:]
    copy.wait()


def place_tokens(q, p, rows):
    vmem = pl.BlockSpec(memory_space=pltpu.VMEM)
    shape = (NY * NX // GROUP, rows, GROUP * BLOCK)
    return pl.pallas_call(
        lambda *refs: place_kernel(len(q), *refs),
        out_shape=(
            jax.ShapeDtypeStruct((HALF, *shape[1:]), jnp.bfloat16),
            jax.ShapeDtypeStruct((HALF, *shape[1:]), jnp.bfloat16),
            jax.ShapeDtypeStruct((rows, BLOCK), jnp.float32),
        ),
        in_specs=[vmem] * (len(q) + len(p)),
        out_specs=(pl.BlockSpec(memory_space=pltpu.HBM), vmem, vmem),
        scratch_shapes=[pltpu.VMEM(shape, jnp.bfloat16), pltpu.SemaphoreType.DMA],
        cost_estimate=pl.CostEstimate(flops=2 * rows * 4096, bytes_accessed=2 * rows * 4096, transcendentals=0),
        compiler_params=pltpu.CompilerParams(vmem_limit_bytes=8 * 1024 * 1024),
        name="place",
    )(*q, *p)


def rows_of(ref, n):
    part = ref[n * GROUP : (n + 1) * GROUP]
    return part.reshape(GROUP * BLOCK, part.shape[2])


def store(held, outs, n, core, sems):
    chips = pl.ds(n * GROUP, GROUP)
    copies = []
    for m, out in enumerate(outs):
        width = out.shape[3]
        copy = pltpu.make_async_copy(
            held.at[chips, :, pl.ds(m * width, width)], out.at[chips, core], sems.at[2 * n + m]
        )
        copy.start()
        copies.append(copy)
    return copies


def own_kernel(w_ref, tok_ref, gate_out, up_out, acc, held, tok, load_sems, sems):
    c = lax.axis_index("c")
    loads, stores = [], []
    for n in range(HALF):
        chips = pl.ds(n * GROUP, GROUP)
        loads.append(pltpu.make_async_copy(w_ref.at[chips], held.at[chips], load_sems.at[2 * n]))
        loads.append(pltpu.make_async_copy(tok_ref.at[n], tok.at[n], load_sems.at[2 * n + 1]))
    for copy in loads:
        copy.start()
    for n in range(HALF):
        loads[2 * n].wait()
        loads[2 * n + 1].wait()
        stores += store(held, (gate_out, up_out), n, c, sems)
        product = jnp.dot(tok[n], rows_of(held, n), preferred_element_type=jnp.float32)
        acc[...] = product if n == 0 else acc[...] + product
    for copy in stores:
        copy.wait()


def other_kernel(w_ref, tok, so_far, square, gate_in, up_in, gate_out, up_out, hidden_ref, acc, sems):
    c = lax.axis_index("c")
    width = hidden_ref.shape[1]
    stores = []
    for n in range(HALF):
        stores += store(w_ref, (gate_out, up_out), n, 1 - c, sems)
    depth = 2 * NZ * BLOCK
    norm = lax.rsqrt(jnp.sum(square[...], axis=1, keepdims=True) / depth + 1e-06) * depth ** (-0.5)
    acc[...] = so_far[...] + jnp.dot(tok[0], rows_of(w_ref, 0), preferred_element_type=jnp.float32)
    total = acc[...] + jnp.dot(tok[1], rows_of(w_ref, 1), preferred_element_type=jnp.float32)
    gate = total[:, :width] * norm
    up = total[:, width:] * norm
    hidden_ref[...] = (gate / (1.0 + jnp.exp(-gate)) * up).astype(hidden_ref.dtype)
    for copy in stores:
        copy.wait()


def products(gathered, crossed, kept, tok, square):
    rows, both = square.shape[0], gathered.shape[1]
    width = both // 2
    vmem = pl.BlockSpec(memory_space=pltpu.VMEM)
    hbm = pl.BlockSpec(memory_space=pltpu.HBM)
    serve = jax.ShapeDtypeStruct((NZ, 2, BLOCK, width), jnp.bfloat16)
    shape = (NZ, BLOCK, both)
    cost = pl.CostEstimate(
        flops=2 * rows * NZ * BLOCK * both, bytes_accessed=4 * NZ * BLOCK * both, transcendentals=0
    )
    gate, up, so_far = pl.pallas_call(
        own_kernel,
        out_shape=(serve, serve, jax.ShapeDtypeStruct((rows, both), jnp.float32)),
        in_specs=[hbm, hbm],
        out_specs=(hbm, hbm, vmem),
        scratch_shapes=[
            pltpu.VMEM(shape, jnp.bfloat16),
            pltpu.VMEM(kept.shape, jnp.bfloat16),
            pltpu.SemaphoreType.DMA((2 * HALF,)),
            pltpu.SemaphoreType.DMA((2 * HALF,)),
        ],
        cost_estimate=cost,
        compiler_params=pltpu.CompilerParams(vmem_limit_bytes=LIMIT_A * 1024 * 1024),
        name="own_rows",
    )(gathered.reshape(shape), kept)
    gate, up, hidden = pl.pallas_call(
        other_kernel,
        out_shape=(serve, serve, jax.ShapeDtypeStruct((rows, width), jnp.bfloat16)),
        in_specs=[vmem, vmem, vmem, vmem, hbm, hbm],
        out_specs=(hbm, hbm, vmem),
        scratch_shapes=[pltpu.VMEM((rows, both), jnp.float32), pltpu.SemaphoreType.DMA((2 * HALF,))],
        input_output_aliases={4: 0, 5: 1},
        cost_estimate=cost,
        compiler_params=pltpu.CompilerParams(vmem_limit_bytes=LIMIT_B * 1024 * 1024),
        name="other_rows",
    )(crossed.reshape(shape), tok, so_far, square, gate, up)
    depth = 2 * NZ * BLOCK
    return gate.reshape(depth, width), up.reshape(depth, width), hidden


def inner(tokens, norm_gain, gate_train, up_train):
    own = rounded(gate_train, up_train, norm_gain)
    gathered = lax.all_gather(own, "z", axis=0, tiled=True)
    crossed = lax.ppermute(gathered, "c", SWAP)

    p0, q0 = tokens[None, :ROWS_P], tokens[None, ROWS_P:]
    pair = jnp.concatenate([p0, lax.ppermute(p0, "x", pairs_of(NX, 0))], 0)
    p4 = jnp.concatenate([pair, lax.ppermute(pair, "x", pairs_of(NX, 1))], 0)
    p = spread_y(p4, 1)
    q8 = jnp.concatenate(spread_y(q0, 0), 0)
    qa = lax.ppermute(q8, "x", pairs_of(NX, 0))
    qb = lax.ppermute(q8, "x", pairs_of(NX, 1))
    qc = lax.ppermute(qb, "x", pairs_of(NX, 0))
    kept, tok, square = place_tokens([q8, qa, qb, qc], p, tokens.shape[0])
    return products(gathered, crossed, kept, tok, square)


def solution(mesh):
    split = Mesh(mesh.devices.reshape(NZ, 2, NY, NX), ("z", "c", "y", "x"))
    fs, tp = ("z", "c"), ("y", "x")
    placed = (P(fs, tp), P(fs), P(fs, tp), P(fs, tp))
    return jax.shard_map(
        inner,
        mesh=split,
        in_specs=placed,
        out_specs=(P(None, tp), P(None, tp), P(fs, tp)),
        check_vma=False,
    )
```

```python
import jax
import jax.numpy as jnp
from jax import lax
from jax.experimental import pallas as pl
from jax.experimental.pallas import tpu as pltpu
from jax.sharding import Mesh
from jax.sharding import PartitionSpec as P


NZ, NY, NX = 16, 8, 4
ROWS_P = 256
BLOCK = 128
GROUP = 8
KEPT = 2


def pairs_of(n, kind):
    return [(i, (i ^ 1) if kind == 0 else ((i - 1) % n if i % 2 == 0 else (i + 1) % n)) for i in range(n)]


def spread_y(own, kind):
    first = lax.ppermute(own, "y", pairs_of(NY, kind))
    pair = jnp.concatenate([own, first], 0)
    second = lax.ppermute(pair, "y", pairs_of(NY, 1 - kind))
    third = lax.ppermute(second, "y", pairs_of(NY, kind))
    fourth = lax.ppermute(third, "y", pairs_of(NY, 1 - kind))
    return [pair, second, third, fourth]


def partner(v, n, kind):
    odd = lax.rem(v, 2)
    return v + 1 - 2 * odd if kind == 0 else lax.rem(v + n - 1 + 2 * odd, n)


def y_order(y, kind):
    f = lambda v: partner(v, NY, kind)
    g = lambda v: partner(v, NY, 1 - kind)
    heads = [y, g(y), g(f(y)), g(f(g(y)))]
    return [v for head in heads for v in (head, f(head))]


def x_order(x):
    far = partner(x, NX, 1)
    return [x, partner(x, NX, 0), far, partner(far, NX, 0)]


def round_kernel(gate_ref, up_ref, gain_ref, out_ref):
    width = gate_ref.shape[1]
    gain = jnp.transpose(jnp.broadcast_to(gain_ref[...], (BLOCK, BLOCK)))
    for n in range(width // BLOCK):
        lanes = pl.ds(n * BLOCK, BLOCK)
        out_ref[:, lanes] = (gate_ref[:, lanes] * gain).astype(out_ref.dtype)
        out_ref[:, pl.ds(width + n * BLOCK, BLOCK)] = (up_ref[:, lanes] * gain).astype(out_ref.dtype)


def rounded(gate, up, gain):
    vmem = pl.BlockSpec(memory_space=pltpu.VMEM)
    return pl.pallas_call(
        round_kernel,
        out_shape=jax.ShapeDtypeStruct((gate.shape[0], 2 * gate.shape[1]), jnp.bfloat16),
        in_specs=[vmem] * 3,
        out_specs=vmem,
        cost_estimate=pl.CostEstimate(flops=2 * gate.size, bytes_accessed=12 * gate.size, transcendentals=0),
        name="round",
    )(gate, up, gain[None, :])


def place_kernel(n_q, *refs):
    q_refs, refs = refs[:n_q], refs[n_q:]
    *p_refs, kept, tok_out, square, tok, sem = refs
    y, x = lax.axis_index("y"), lax.axis_index("x")
    rows_p = p_refs[0].shape[1]
    square[...] = jnp.zeros_like(square)

    def place(ref, at, row, ty, tx):
        t = ty * NX + tx
        lane = pl.multiple_of(lax.rem(t, GROUP) * BLOCK, BLOCK)
        value = ref[at]
        span = pl.ds(row, value.shape[0])
        tok[lax.div(t, GROUP), span, pl.ds(lane, BLOCK)] = value
        wide = value.astype(jnp.float32)
        square[span, :] += wide * wide

    xs = x_order(x)
    ys = y_order(y, 0)
    for i, r in enumerate(q_refs):
        for j in range(NY):
            place(r, j, rows_p, ys[j], xs[i])
    ys = y_order(y, 1)
    at = 0
    for r in p_refs:
        for j in range(r.shape[0]):
            place(r, j, 0, ys[(at + j) // NX], xs[(at + j) % NX])
        at += r.shape[0]
    copy = pltpu.make_async_copy(tok.at[pl.ds(KEPT, tok_out.shape[0])], tok_out, sem)
    copy.start()
    kept[...] = tok[:KEPT]
    copy.wait()


def place_tokens(q, p, rows):
    vmem = pl.BlockSpec(memory_space=pltpu.VMEM)
    shape = (NY * NX // GROUP, rows, GROUP * BLOCK)
    return pl.pallas_call(
        lambda *refs: place_kernel(len(q), *refs),
        out_shape=(
            jax.ShapeDtypeStruct((KEPT, *shape[1:]), jnp.bfloat16),
            jax.ShapeDtypeStruct((shape[0] - KEPT, *shape[1:]), jnp.bfloat16),
            jax.ShapeDtypeStruct((rows, BLOCK), jnp.float32),
        ),
        in_specs=[vmem] * (len(q) + len(p)),
        out_specs=(vmem, pl.BlockSpec(memory_space=pltpu.HBM), vmem),
        scratch_shapes=[pltpu.VMEM(shape, jnp.bfloat16), pltpu.SemaphoreType.DMA],
        cost_estimate=pl.CostEstimate(flops=2 * rows * 4096, bytes_accessed=2 * rows * 4096, transcendentals=0),
        compiler_params=pltpu.CompilerParams(vmem_limit_bytes=8 * 1024 * 1024),
        name="place",
    )(*q, *p)


def last_kernel(
    w_ref, kept, tok_ref, square, gate_out, up_out, hidden_out, held, tok, acc, hidden, sems
):
    width = hidden_out.shape[1]
    pieces, span = NY * NX // GROUP, GROUP * BLOCK
    loads, stores = [[] for _ in range(pieces)], []
    for n in range(pieces):
        rows = pl.ds(n * span, span)
        loads[n].append(pltpu.make_async_copy(w_ref.at[rows], held.at[rows], sems.at[4 * n]))
        if n >= KEPT:
            loads[n].append(
                pltpu.make_async_copy(tok_ref.at[n - KEPT], tok.at[n - KEPT], sems.at[4 * n + 1])
            )
        for m, out in enumerate((gate_out, up_out)):
            stores.append(
                pltpu.make_async_copy(
                    held.at[rows, pl.ds(m * width, width)], out.at[rows], sems.at[4 * n + 2 + m]
                )
            )
    for group in loads:
        for copy in group:
            copy.start()
    depth = w_ref.shape[0]
    norm = lax.rsqrt(jnp.sum(square[...], axis=1, keepdims=True) / depth + 1e-06) * depth ** (-0.5)
    for n in range(pieces):
        for copy in loads[n]:
            copy.wait()
        if n > 0:
            for copy in stores[2 * n - 2 : 2 * n]:
                copy.start()
        features = kept.at[n] if n < KEPT else tok.at[n - KEPT]
        weights = held[pl.ds(n * span, span), :]
        if n < pieces - 1:
            product = jnp.dot(features[...], weights, preferred_element_type=jnp.float32)
            acc[...] = product if n == 0 else acc[...] + product
    for copy in stores[2 * pieces - 2 :]:
        copy.start()
    half = hidden_out.shape[0] // 2
    for m in range(2):
        rows = pl.ds(m * half, half)
        product = acc[rows, :] + jnp.dot(features[rows, :], weights, preferred_element_type=jnp.float32)
        gate = product[:, :width] * norm[m * half : (m + 1) * half]
        up = product[:, width:] * norm[m * half : (m + 1) * half]
        hidden[rows, :] = (gate / (1.0 + jnp.exp(-gate)) * up).astype(hidden.dtype)
        stores.append(pltpu.make_async_copy(hidden.at[rows], hidden_out.at[rows], sems.at[4 * pieces + m]))
        stores[-1].start()
    for copy in stores:
        copy.wait()


def last_part(gathered, kept, tok, square):
    depth, both = gathered.shape
    rows, width = square.shape[0], both // 2
    vmem = pl.BlockSpec(memory_space=pltpu.VMEM)
    hbm = pl.BlockSpec(memory_space=pltpu.HBM)
    return pl.pallas_call(
        last_kernel,
        out_shape=(
            jax.ShapeDtypeStruct((depth, width), jnp.bfloat16),
            jax.ShapeDtypeStruct((depth, width), jnp.bfloat16),
            jax.ShapeDtypeStruct((rows, width), jnp.bfloat16),
        ),
        in_specs=[hbm, vmem, hbm, vmem],
        out_specs=(hbm, hbm, hbm),
        scratch_shapes=[
            pltpu.VMEM((depth, both), jnp.bfloat16),
            pltpu.VMEM(tok.shape, jnp.bfloat16),
            pltpu.VMEM((rows, both), jnp.float32),
            pltpu.VMEM((rows, width), jnp.bfloat16),
            pltpu.SemaphoreType.DMA((32,)),
        ],
        cost_estimate=pl.CostEstimate(
            flops=4 * rows * depth * width, bytes_accessed=6 * depth * both, transcendentals=rows * width
        ),
        compiler_params=pltpu.CompilerParams(vmem_limit_bytes=51 * 1024 * 1024),
        name="last",
    )(gathered, kept, tok, square)


def inner(tokens, norm_gain, gate_train, up_train):
    own = rounded(gate_train, up_train, norm_gain)
    gathered = lax.all_gather(own, ("z", "c"), axis=0, tiled=True)

    p0, q0 = tokens[None, :ROWS_P], tokens[None, ROWS_P:]
    pair = jnp.concatenate([p0, lax.ppermute(p0, "x", pairs_of(NX, 0))], 0)
    p4 = jnp.concatenate([pair, lax.ppermute(pair, "x", pairs_of(NX, 1))], 0)
    p = spread_y(p4, 1)
    q8 = jnp.concatenate(spread_y(q0, 0), 0)
    qa = lax.ppermute(q8, "x", pairs_of(NX, 0))
    qb = lax.ppermute(q8, "x", pairs_of(NX, 1))
    qc = lax.ppermute(qb, "x", pairs_of(NX, 0))
    kept, tok, square = place_tokens([q8, qa, qb, qc], p, tokens.shape[0])
    return last_part(gathered, kept, tok, square)


def solution(mesh):
    split = Mesh(mesh.devices.reshape(NZ, 2, NY, NX), ("z", "c", "y", "x"))
    fs, tp = ("z", "c"), ("y", "x")
    placed = (P(fs, tp), P(fs), P(fs, tp), P(fs, tp))
    return jax.shard_map(
        inner,
        mesh=split,
        in_specs=placed,
        out_specs=(P(None, tp), P(None, tp), P(fs, tp)),
        check_vma=False,
    )
```
